32 devices in a mesh: ep: 8 (over z, x), tp: 4 (over y, core).
Axes of the slice: x: 2, y: 2, z: 4, core: 2. Of those that a mesh axis runs over, the one named last changes fastest.
Arguments:
- tokens: bfloat16 [512, 2048], P('ep'), may hold values from -6 to 6
- norm_gain: float32 [2048], replicated, may hold values from 0.1 to 1.9
- norm_shift: float32 [2048], replicated, may hold values from -3 to 3
- expert_ids: int32 [512, 4], P('ep'), may hold values from 0 to 15, as said below
- gate_weights: float32 [512, 4], P('ep'), may hold values from 0.1 to 1
- expert_gate: bfloat16 [16, 2048, 512], P('ep', None, 'tp'), may hold values from -0.125 to 0.125
- expert_up: bfloat16 [16, 2048, 512], P('ep', None, 'tp'), may hold values from -0.125 to 0.125
- expert_down: bfloat16 [16, 512, 2048], P('ep', 'tp'), may hold values from -0.25 to 0.25
Outputs:
- mixed_out: bfloat16 [512, 2048], P('ep', 'tp')
The draws below stay inside these ranges and needn't reach their ends.
Inputs may be any that keep to these rules, and one draw needn't show every extreme that they name: `expert_ids`: each row names 4 distinct experts that all lie in one group of 4 consecutive expert numbers. In the rows of one index of ep (aligned blocks of 64 rows) no expert is named by more than 32 rows, and in every block some expert is named by exactly 32 rows.
All inputs are finite; a program needn't handle non-finite values.
Results may differ from the reference program's by a relative error of at most 0.002.
Values may be sent and summed in bfloat16 or wider, within the bound.
A program may use at most 64 MiB of HBM per device.

```python
import jax
import jax.numpy as jnp
from jax import lax

D = 2048
F = 512
TOP_K = 4
GROUPS = 4
TOK_DEV = 64
EXPERTS = 16
GROUP_SIZE = 4
CAP = 32
TOKENS = 512
N_EP = 8


def shuffle_block(block_key):
    return jax.random.permutation(block_key, TOK_DEV)


def draw_expert_ids(key, part):
    key_heavy = jax.random.fold_in(key, 11)
    key_order = jax.random.fold_in(key, 23)
    key_shift = jax.random.fold_in(key, 37)
    heavy = jax.random.randint(key_heavy, (N_EP, 1), 0, GROUPS)
    block_keys = jax.random.split(key_order, N_EP)
    order = jax.vmap(shuffle_block)(block_keys).astype(jnp.int32)
    inverse = jnp.argsort(order, axis=1).astype(jnp.int32)
    half_rows = TOK_DEV // 2
    others = jnp.maximum(inverse - half_rows, 0)
    in_heavy = inverse < half_rows
    group_id = jnp.where(in_heavy, heavy, (heavy + 1 + others % (GROUPS - 1)) % GROUPS)
    ranks = jnp.where(in_heavy, inverse, others // (GROUPS - 1))
    offsets = jax.random.randint(key_shift, (N_EP, GROUPS), 0, GROUP_SIZE)
    shift_rows = jnp.take_along_axis(offsets, group_id, axis=1)
    within = (ranks[:, :, None] * TOP_K + jnp.arange(TOP_K, dtype=jnp.int32)[None, None, :] + shift_rows[:, :, None]) % GROUP_SIZE
    chosen = group_id[:, :, None] * GROUP_SIZE + within
    return chosen.reshape(N_EP * TOK_DEV, TOP_K).astype(jnp.int32)


def levels(key, extent, shards, least, top_value):
    gain = 1.0
    for axis_at, parts in shards:
        steps = jax.random.uniform(jax.random.fold_in(jax.random.fold_in(key, 6), axis_at), (parts,), jnp.float32, least / len(shards), top_value / len(shards))
        gain = gain * jnp.repeat(jnp.exp(steps), extent[axis_at] // parts).reshape((-1,) + (1,) * (len(extent) - 1 - axis_at))
    return gain


def normal_values(own_key, dims, width, limit, shards=(), kind=jnp.bfloat16):
    values = jax.random.normal(own_key, dims, jnp.float32) * width
    if len(shards) > 0:
        values = levels(own_key, dims, shards, -0.22, 0.18) * values
    return jnp.clip(values, min=-limit, max=limit).astype(kind)


def setup_inputs(seed: int = 0) -> dict:
    keys = jax.random.split(jax.random.key(seed), 9)
    tokens = normal_values(keys[0], (TOKENS, D), 1.0, 6.0, ((0, 8),))
    norm_gain = jnp.clip(1.0 + 0.18 * jax.random.normal(keys[1], (D,), jnp.float32), 0.1, 1.9)
    norm_shift = normal_values(keys[2], (D,), 0.5, 3.0, (), jnp.float32)
    expert_ids = draw_expert_ids(jax.random.fold_in(keys[8], 71), 0)
    gate_weights = jnp.clip(0.1 + 0.9 * jax.random.uniform(keys[4], (TOKENS, TOP_K), jnp.float32) ** levels(keys[4], (TOKENS, TOP_K), ((0, 8),), -0.2, 0.2), 0.1, 1.0)
    expert_gate = normal_values(keys[5], (EXPERTS, D, F), D ** -0.5, 0.125, ((0, 8), (2, 4)))
    expert_up = normal_values(keys[6], (EXPERTS, D, F), D ** -0.5, 0.125, ((0, 8), (2, 4)))
    expert_down = normal_values(keys[7], (EXPERTS, F, D), F ** -0.5, 0.25, ((0, 8), (1, 4)))
    return {"tokens": tokens, "norm_gain": norm_gain, "norm_shift": norm_shift, "expert_ids": expert_ids, "gate_weights": gate_weights, "expert_gate": expert_gate, "expert_up": expert_up, "expert_down": expert_down}


epsilon = 1e-05

def layer_norm(tokens, norm_gain, norm_shift):
    values = tokens.astype(jnp.float32)
    centre = lax.optimization_barrier(jnp.mean(values, axis=-1, keepdims=True))
    spread = lax.optimization_barrier(jnp.mean(jnp.square(values - centre), axis=-1, keepdims=True))
    scaled = (values - centre) * lax.rsqrt(spread + epsilon) * norm_gain + norm_shift
    return scaled.astype(jnp.bfloat16)

def reference(tokens, norm_gain, norm_shift, expert_ids, gate_weights, expert_gate, expert_up, expert_down):
    normed = layer_norm(tokens, norm_gain, norm_shift)
    bound_rows = N_EP * CAP

    def one_expert(totals, expert):
        hits = expert_ids == expert
        weight_all = lax.optimization_barrier(jnp.sum(jnp.where(hits, gate_weights, jnp.float32(0.0)), axis=1))
        routed = jnp.any(hits, axis=1)
        chosen = jnp.nonzero(routed, size=bound_rows, fill_value=0)[0].astype(jnp.int32)
        valid = (jnp.arange(bound_rows, dtype=jnp.int32) < jnp.sum(routed.astype(jnp.int32))).astype(jnp.float32)
        rows_in = normed[chosen]
        gate_sum = jnp.dot(rows_in, expert_gate[expert], preferred_element_type=jnp.float32)
        upward = jnp.dot(rows_in, expert_up[expert], preferred_element_type=jnp.float32)
        hidden = (jax.nn.silu(gate_sum) * upward).astype(jnp.bfloat16)
        result = jnp.dot(hidden, expert_down[expert], preferred_element_type=jnp.float32)
        scale_rows = weight_all[chosen] * valid
        totals = totals.at[chosen].add(result * scale_rows[:, None])
        return (totals, None)
    start_sum = jnp.zeros((TOKENS, D), jnp.float32)
    totals, _ = lax.scan(one_expert, start_sum, jnp.arange(EXPERTS, dtype=jnp.int32))
    return totals.astype(jnp.bfloat16)
```

```python
import functools

import jax
import jax.numpy as jnp
from jax import lax
from jax.experimental import pallas as pl
from jax.experimental.pallas import tpu as pltpu
from jax.sharding import PartitionSpec as P

GROUPS = 4
CORES = 2
EPSILON = 1e-05
MESH = pl.DeviceIdType.MESH


def kernel(
    ep_size, tp_size,
    tok_ref, gain_ref, shift_ref, ids_ref, gw_ref, wg_ref, wu_ref, wd_ref, out_ref,
    x_buf, xs_buf, sel_buf, wall_buf, wr_buf, wcat, wdn, acc,
    r1_send, r1_recv, r1_own, r2_send, r2_recv, f_send, f_recv,
    w_sem, s1_s, s1_r, wt_s, wt_r, a_s, a_r, b_s, b_r, c1_s, c1_r, c2_s, c2_r, c3_s, c3_r,
):
    tok_rows, features = tok_ref.shape
    local, _, units = wg_ref.shape
    top_k = ids_ref.shape[1]
    members = ep_size // GROUPS
    rows_tp = tp_size // CORES
    group_size = local * members
    half = tok_rows // 2
    quarter = features // tp_size
    lanes = GROUPS * half
    parts, _, width = wcat.shape

    e = lax.axis_index("ep")
    j = lax.axis_index("tp")
    gme, m = e // members, e % members
    y, c = j // CORES, j % CORES
    partner = {"ep": e, "tp": y * CORES + (1 - c)}
    others = [(dm, dy) for dm in range(members) for dy in range(rows_tp) if dm or dy]
    slots = others + [(0, 0)]
    own = len(others)

    def ahead(k):
        dm, dy = slots[k]
        return lax.rem(m + dm, members), lax.rem(y + dy, rows_tp)

    def behind(k):
        dm, dy = slots[k]
        return lax.rem(m + members - dm, members), lax.rem(y + rows_tp - dy, rows_tp)

    def block_at(db):
        return lax.rem(gme + GROUPS - db, GROUPS)

    def remote(src, dst, ssem, rsem, dev):
        return pltpu.make_async_remote_copy(
            src_ref=src, dst_ref=dst, send_sem=ssem, recv_sem=rsem,
            device_id=dev, device_id_type=MESH,
        )

    sent = []

    def start(*args):
        copy = remote(*args)
        copy.start()
        sent.append(copy)

    barrier = pltpu.get_barrier_semaphore()
    greeted = 0
    for d in range(1, ep_size):
        pl.semaphore_signal(
            barrier, inc=1, device_id={"ep": lax.rem(e + d, ep_size), "tp": j}, device_id_type=MESH
        )
        greeted += 1
    for k, (dm, dy) in enumerate(others):
        if dy:
            mm, yy = ahead(k)
            pl.semaphore_signal(
                barrier, inc=1,
                device_id={"ep": gme * members + mm, "tp": yy * CORES + c}, device_id_type=MESH,
            )
            greeted += 1
    pl.semaphore_signal(barrier, inc=1, device_id=partner, device_id_type=MESH)
    greeted += 1

    weights = []
    for le in range(local):
        for source, at in ((wg_ref, 2 * le * units), (wu_ref, (2 * le + 1) * units)):
            weights.append(
                (source.at[le], wcat.at[at // width, :, pl.ds(at % width, units)])
            )
        for q in range(tp_size):
            weights.append((wd_ref.at[le, :, pl.ds(q * quarter, quarter)], wdn.at[q, le]))
    weights = [pltpu.make_async_copy(s, d, w_sem.at[i]) for i, (s, d) in enumerate(weights)]
    for copy in weights:
        copy.start()

    ids = ids_ref[...]
    group_of = ids[:, 0:1] // group_size
    lane = lax.broadcasted_iota(jnp.int32, (tok_rows, lanes), 1)
    in_group = group_of == lane // half
    earlier = (
        lax.broadcasted_iota(jnp.int32, (tok_rows, tok_rows), 1)
        < lax.broadcasted_iota(jnp.int32, (tok_rows, tok_rows), 0)
    )
    rank = jnp.dot(
        earlier.astype(jnp.float32).astype(jnp.bfloat16),
        in_group.astype(jnp.float32).astype(jnp.bfloat16),
        preferred_element_type=jnp.float32,
    )
    picked = in_group & (rank == (lane % half).astype(jnp.float32))
    sel = picked.astype(jnp.float32)
    sel_bf = sel.astype(jnp.bfloat16)
    sel_buf[...] = sel_bf
    within = ids - group_of * group_size
    gw = gw_ref[...]
    wall_buf[...] = jnp.zeros_like(wall_buf)
    for i in range(group_size):
        mine = jnp.sum(jnp.where(within == i, gw, 0.0), axis=1, keepdims=True)
        wall_buf[i : i + 1, :] = jnp.sum(sel * mine, axis=0, keepdims=True)

    values = tok_ref[...].astype(jnp.float32)
    centre = jnp.mean(values, axis=-1, keepdims=True)
    spread = jnp.mean(jnp.square(values - centre), axis=-1, keepdims=True)
    share = pl.ds(pl.multiple_of(j * quarter, quarter), quarter)
    part = tok_ref[:, share].astype(jnp.float32)
    normed = (
        (part - centre) * lax.rsqrt(spread + EPSILON) * gain_ref[:, share] + shift_ref[:, share]
    ).astype(jnp.bfloat16)
    packed = lax.dot_general(
        sel_bf, normed, (((0,), (0,)), ((), ())), preferred_element_type=jnp.float32
    ).astype(jnp.bfloat16)
    packed = packed.reshape(GROUPS, half, quarter)
    xs_buf[...] = packed

    pl.semaphore_wait(barrier, greeted)

    for dg in range(1, GROUPS):
        g = lax.rem(gme + dg, GROUPS)
        start(
            xs_buf.at[g], x_buf.at[m, j, gme], s1_s.at[dg], s1_r.at[dg],
            {"ep": g * members + m, "tp": j},
        )
    x_buf[m, j, gme] = xs_buf[gme]
    for d in range(1, ep_size):
        start(
            wall_buf, wr_buf.at[e], wt_s.at[d], wt_r.at[d],
            {"ep": lax.rem(e + d, ep_size), "tp": j},
        )
    wr_buf[e] = wall_buf[...]

    for db in range(GROUPS):
        b = block_at(db)
        mine = x_buf.at[m, j, b]
        if db:
            remote(mine, mine, s1_s.at[db], s1_r.at[db], partner).wait_recv()
        for k in range(own):
            mm, yy = ahead(k)
            start(
                mine, mine, a_s.at[db, k], a_r.at[db, k],
                {"ep": gme * members + mm, "tp": yy * CORES + c},
            )
        start(mine, mine, b_s.at[db, own], b_r.at[db, own], partner)
    for db in range(GROUPS):
        b = block_at(db)
        for k in range(own):
            mm, yy = behind(k)
            slot = x_buf.at[mm, yy * CORES + c, b]
            remote(slot, slot, a_s.at[db, k], a_r.at[db, k], partner).wait_recv()
            start(slot, slot, b_s.at[db, k], b_r.at[db, k], partner)

    for copy in weights:
        copy.wait()
    acc[...] = jnp.zeros_like(acc)

    def project(mm, jj):
        rows = x_buf[mm, jj].reshape(lanes, quarter)
        depth = pl.ds(pl.multiple_of(jj * quarter, quarter), quarter)
        for part in range(parts):
            acc[mm, part] += jnp.dot(
                rows, wcat[part, depth, :], preferred_element_type=jnp.float32
            )

    order = [own] + list(range(own))
    for k in order:
        mm, yy = behind(k)
        project(mm, yy * CORES + c)
    for d in range(1, ep_size):
        slot = wr_buf.at[lax.rem(e + ep_size - d, ep_size)]
        remote(slot, slot, wt_s.at[d], wt_r.at[d], partner).wait_recv()
    for k in order:
        mm, yy = behind(k)
        for db in range(GROUPS):
            slot = x_buf.at[mm, yy * CORES + (1 - c), block_at(db)]
            remote(slot, slot, b_s.at[db, k], b_r.at[db, k], partner).wait_recv()
        project(mm, yy * CORES + (1 - c))

    slot_row = lax.broadcasted_iota(jnp.int32, (half, lanes), 0) + gme * half
    slot_lane = lax.broadcasted_iota(jnp.int32, (half, lanes), 1)
    diagonal = slot_row == slot_lane
    hidden, scale = {}, {}
    for dm in range(members):
        mm = lax.rem(m + dm, members)
        for le in range(local):
            at, to = 2 * le * units, (2 * le + 1) * units
            gate = acc[mm, at // width, :, at % width : at % width + units]
            up = acc[mm, to // width, :, to % width : to % width + units]
            hidden[dm, le] = (gate / (1.0 + jnp.exp(-gate)) * up).astype(jnp.bfloat16)
            columns = []
            for b in range(GROUPS):
                row = wr_buf[b * members + mm, pl.ds(m * local + le, 1), :]
                columns.append(jnp.sum(jnp.where(diagonal, row, 0.0), axis=1, keepdims=True))
            scale[dm, le] = jnp.concatenate(columns, axis=0)

    def lower(dm, q):
        total = None
        for le in range(local):
            term = scale[dm, le] * jnp.dot(
                hidden[dm, le], wdn[q, le], preferred_element_type=jnp.float32
            )
            total = term if total is None else total + term
        return total

    for k in range(own + 1):
        _, yy = ahead(k)
        r1_send[k] = lower(slots[k][0], yy * CORES + (1 - c))
        start(r1_send.at[k], r1_recv.at[k], c1_s.at[k], c1_r.at[k], partner)
    for k in range(own + 1):
        _, yy = ahead(k)
        r1_own[k] = lower(slots[k][0], yy * CORES + c)
    for k in range(own + 1):
        mm, yy = ahead(k)
        slot = r1_recv.at[k]
        remote(slot, slot, c1_s.at[k], c1_r.at[k], partner).wait_recv()
        summed = r1_own[k] + r1_recv[k]
        if k < own:
            r2_send[k] = summed
            start(
                r2_send.at[k], r2_recv.at[k], c2_s.at[k], c2_r.at[k],
                {"ep": gme * members + mm, "tp": yy * CORES + c},
            )
    for k in range(own):
        slot = r2_recv.at[k]
        remote(slot, slot, c2_s.at[k], c2_r.at[k], partner).wait_recv()
        summed = summed + r2_recv[k]
    f_send[...] = summed.astype(jnp.bfloat16).reshape(GROUPS, half, quarter)
    for dg in range(1, GROUPS):
        g = lax.rem(gme + dg, GROUPS)
        start(
            f_send.at[g], f_recv.at[gme], c3_s.at[dg], c3_r.at[dg],
            {"ep": g * members + m, "tp": j},
        )
    f_recv[gme] = f_send[gme]
    for dg in range(1, GROUPS):
        slot = f_recv.at[block_at(dg)]
        remote(slot, slot, c3_s.at[dg], c3_r.at[dg], partner).wait_recv()
    out_ref[...] = jnp.dot(
        sel_buf[...], f_recv[...].reshape(lanes, quarter), preferred_element_type=jnp.float32
    ).astype(jnp.bfloat16)
    for copy in sent:
        copy.wait_send()


def per_device(tokens, norm_gain, norm_shift, expert_ids, gate_weights, w_gate, w_up, w_down):
    ep_size, tp_size = lax.axis_size("ep"), lax.axis_size("tp")
    tok_rows, features = tokens.shape
    local, _, units = w_gate.shape
    members, rows_tp = ep_size // GROUPS, tp_size // CORES
    half, quarter = tok_rows // 2, features // tp_size
    lanes = GROUPS * half
    group_size = local * members
    padded = -(-group_size // 8) * 8
    chunks = members * rows_tp
    parts, width = (1, 2 * local * units) if units % 128 == 0 else (2 * local, units)
    bf16, f32 = jnp.bfloat16, jnp.float32
    dma = pltpu.SemaphoreType.DMA
    vmem = pl.BlockSpec(memory_space=pltpu.VMEM)
    hbm = pl.BlockSpec(memory_space=pl.ANY)
    return pl.pallas_call(
        functools.partial(kernel, ep_size, tp_size),
        out_shape=jax.ShapeDtypeStruct((tok_rows, quarter), bf16),
        in_specs=[vmem] * 5 + [hbm] * 3,
        out_specs=vmem,
        scratch_shapes=[
            pltpu.VMEM((members, tp_size, GROUPS, half, quarter), bf16),
            pltpu.VMEM((GROUPS, half, quarter), bf16),
            pltpu.VMEM((tok_rows, lanes), bf16),
            pltpu.VMEM((padded, lanes), f32),
            pltpu.VMEM((ep_size, padded, lanes), f32),
            pltpu.VMEM((parts, features, width), bf16),
            pltpu.VMEM((tp_size, local, units, quarter), bf16),
            pltpu.VMEM((members, parts, lanes, width), f32),
            pltpu.VMEM((chunks, lanes, quarter), f32),
            pltpu.VMEM((chunks, lanes, quarter), f32),
            pltpu.VMEM((chunks, lanes, quarter), f32),
            pltpu.VMEM((chunks, lanes, quarter), f32),
            pltpu.VMEM((chunks, lanes, quarter), f32),
            pltpu.VMEM((GROUPS, half, quarter), bf16),
            pltpu.VMEM((GROUPS, half, quarter), bf16),
            dma((local * (2 + tp_size),)),
            dma((GROUPS,)), dma((GROUPS,)),
            dma((ep_size,)), dma((ep_size,)),
            dma((GROUPS, chunks)), dma((GROUPS, chunks)),
            dma((GROUPS, chunks)), dma((GROUPS, chunks)),
            dma((chunks,)), dma((chunks,)),
            dma((chunks,)), dma((chunks,)),
            dma((GROUPS,)), dma((GROUPS,)),
        ],
        compiler_params=pltpu.CompilerParams(
            collective_id=0, has_side_effects=True, vmem_limit_bytes=48 * 1024 * 1024
        ),
    )(
        tokens, norm_gain.reshape(1, features), norm_shift.reshape(1, features),
        expert_ids, gate_weights, w_gate, w_up, w_down,
    )


def solution(mesh):
    return jax.shard_map(
        per_device,
        mesh=mesh,
        in_specs=(
            P("ep", None),
            P(),
            P(),
            P("ep", None),
            P("ep", None),
            P("ep", None, "tp"),
            P("ep", None, "tp"),
            P("ep", "tp", None),
        ),
        out_specs=P("ep", "tp"),
        check_vma=False,
    )
```

```python
import functools

import jax
import jax.numpy as jnp
from jax import lax
from jax.experimental import pallas as pl
from jax.experimental.pallas import tpu as pltpu
from jax.sharding import PartitionSpec as P

GROUPS = 4
CORES = 2
STAGES = 2
LEVELS = 32000.0
EPSILON = 1e-05
MESH = pl.DeviceIdType.MESH


def kernel(
    ep_size, tp_size,
    tok_hbm, gain_hbm, shift_hbm, ids_hbm, gw_hbm, wg_ref, wu_ref, wd_ref, out_ref,
    tok_ref, gain_ref, shift_ref, ids_ref, gw_ref,
    x_buf, xs_buf, sel_buf, wall_buf, wr_buf, wcat, wdn, acc,
    r1_send, r1_recv, r1_own, q_send, q_recv, u_send, u_recv, f_send, f_recv,
    in_sem, w_sem, s1_s, s1_r, wt_s, wt_r, a_s, a_r, b_s, b_r,
    c1_s, c1_r, c2_s, c2_r, cu_s, cu_r, c3_s, c3_r,
):
    tok_rows, features = tok_ref.shape
    local, _, units = wg_ref.shape
    top_k = ids_ref.shape[0]
    members = ep_size // GROUPS
    rows_tp = tp_size // CORES
    group_size = local * members
    half = tok_rows // 2
    quarter = features // tp_size
    lanes = GROUPS * half
    parts, _, width = wcat.shape
    per_stage = GROUPS // STAGES
    rows = per_stage * half
    scale_lanes = u_send.shape[-1]

    e = lax.axis_index("ep")
    j = lax.axis_index("tp")
    gme, m = e // members, e % members
    y, c = j // CORES, j % CORES
    partner = {"ep": e, "tp": y * CORES + (1 - c)}
    others = [(dm, dy) for dy in reversed(range(rows_tp)) for dm in reversed(range(members)) if dm or dy]
    chunk_of = {at: k for k, at in enumerate(others)}
    own = len(others)
    chunk_of[0, 0] = own

    def ahead(dm, dy):
        return lax.rem(m + dm, members), lax.rem(y + dy, rows_tp)

    def behind(dm, dy):
        return lax.rem(m + members - dm, members), lax.rem(y + rows_tp - dy, rows_tp)

    def member(dm, dy):
        mm, yy = ahead(dm, dy)
        return {"ep": gme * members + mm, "tp": yy * CORES + c}

    def block_at(db):
        return lax.rem(gme + GROUPS - db, GROUPS)

    def remote(src, dst, ssem, rsem, dev):
        return pltpu.make_async_remote_copy(
            src_ref=src, dst_ref=dst, send_sem=ssem, recv_sem=rsem,
            device_id=dev, device_id_type=MESH,
        )

    sent = []

    def start(*args):
        copy = remote(*args)
        copy.start()
        sent.append(copy)

    def arrive(slot, ssem, rsem):
        remote(slot, slot, ssem, rsem, partner).wait_recv()

    inputs = [
        pltpu.make_async_copy(s, d, in_sem.at[i])
        for i, (s, d) in enumerate([
            (ids_hbm, ids_ref), (gw_hbm, gw_ref), (tok_hbm, tok_ref),
            (gain_hbm, gain_ref), (shift_hbm, shift_ref),
        ])
    ]
    for copy in inputs:
        copy.start()

    barrier = pltpu.get_barrier_semaphore()
    greeted = 0
    for d in range(1, ep_size):
        pl.semaphore_signal(
            barrier, inc=1, device_id={"ep": lax.rem(e + d, ep_size), "tp": j}, device_id_type=MESH
        )
        greeted += 1
    for dm, dy in others:
        if dy:
            pl.semaphore_signal(barrier, inc=1, device_id=member(dm, dy), device_id_type=MESH)
            greeted += 1
    pl.semaphore_signal(barrier, inc=1, device_id=partner, device_id_type=MESH)
    greeted += 1

    weights = []
    for le in range(local):
        for source, at in ((wg_ref, 2 * le * units), (wu_ref, (2 * le + 1) * units)):
            weights.append(
                (source.at[le], wcat.at[at // width, :, pl.ds(at % width, units)])
            )
        for q in range(tp_size):
            weights.append((wd_ref.at[le, :, pl.ds(q * quarter, quarter)], wdn.at[q, le]))
    weights = [pltpu.make_async_copy(s, d, w_sem.at[i]) for i, (s, d) in enumerate(weights)]
    for copy in weights:
        copy.start()

    for copy in inputs[:2]:
        copy.wait()
    square = (tok_rows, tok_rows)
    token_at = lax.broadcasted_iota(jnp.int32, square, 0)
    other_at = lax.broadcasted_iota(jnp.int32, square, 1)
    ids = [
        jnp.sum(jnp.where(token_at == other_at, ids_ref[k : k + 1, :], 0), axis=1, keepdims=True)
        for k in range(top_k)
    ]
    gw = [
        jnp.sum(jnp.where(token_at == other_at, gw_ref[k : k + 1, :], 0.0), axis=1, keepdims=True)
        for k in range(top_k)
    ]
    group_of = ids[0] // group_size
    lane = lax.broadcasted_iota(jnp.int32, (tok_rows, lanes), 1)
    in_group = group_of == lane // half
    rank = jnp.dot(
        (other_at < token_at).astype(jnp.float32).astype(jnp.bfloat16),
        in_group.astype(jnp.float32).astype(jnp.bfloat16),
        preferred_element_type=jnp.float32,
    )
    picked = in_group & (rank == (lane % half).astype(jnp.float32))
    sel = picked.astype(jnp.float32)
    sel_bf = sel.astype(jnp.bfloat16)
    sel_buf[...] = sel_bf

    for copy in inputs[2:]:
        copy.wait()
    values = tok_ref[...].astype(jnp.float32)
    centre = jnp.mean(values, axis=-1, keepdims=True)
    spread = jnp.mean(jnp.square(values - centre), axis=-1, keepdims=True)
    share = pl.ds(pl.multiple_of(j * quarter, quarter), quarter)
    part = tok_ref[:, share].astype(jnp.float32)
    normed = (
        (part - centre) * lax.rsqrt(spread + EPSILON) * gain_ref[:, share] + shift_ref[:, share]
    ).astype(jnp.bfloat16)
    packed = lax.dot_general(
        sel_bf, normed, (((0,), (0,)), ((), ())), preferred_element_type=jnp.float32
    ).astype(jnp.bfloat16)
    xs_buf[...] = packed.reshape(GROUPS, half, quarter)

    pl.semaphore_wait(barrier, greeted)

    for dg in range(1, GROUPS):
        g = lax.rem(gme + dg, GROUPS)
        start(
            xs_buf.at[g], x_buf.at[m, j, dg], s1_s.at[dg], s1_r.at[dg],
            {"ep": g * members + m, "tp": j},
        )
    x_buf[m, j, 0] = xs_buf[gme]

    def spread_block(db):
        mine = x_buf.at[m, j, db]
        for k, (dm, dy) in enumerate(others):
            start(mine, mine, a_s.at[db, k], a_r.at[db, k], member(dm, dy))
        start(mine, mine, b_s.at[db, own], b_r.at[db, own], partner)

    spread_block(0)
    wall_buf[...] = jnp.zeros_like(wall_buf)
    for i in range(group_size):
        mine = 0.0
        for k in range(top_k):
            mine = mine + jnp.where(ids[k] - group_of * group_size == i, gw[k], 0.0)
        wall_buf[i : i + 1, :] = jnp.sum(sel * mine, axis=0, keepdims=True)
    for d in range(1, ep_size):
        start(
            wall_buf, wr_buf.at[e], wt_s.at[d], wt_r.at[d],
            {"ep": lax.rem(e + d, ep_size), "tp": j},
        )
    wr_buf[e] = wall_buf[...]
    for db in range(1, GROUPS):
        arrive(x_buf.at[m, j, db], s1_s.at[db], s1_r.at[db])
        spread_block(db)

    slot_row = lax.broadcasted_iota(jnp.int32, (half, lanes), 0) + gme * half
    diagonal = slot_row == lax.broadcasted_iota(jnp.int32, (half, lanes), 1)
    scale_eye = (
        lax.broadcasted_iota(jnp.int32, (rows, scale_lanes), 0)
        == lax.broadcasted_iota(jnp.int32, (rows, scale_lanes), 1)
    )

    def project(jj, blocks):
        held = [
            x_buf[lax.rem(m + dm, members), jj, db] for dm in range(members) for db in blocks
        ]
        held = jnp.concatenate(held, axis=0)
        depth = pl.ds(pl.multiple_of(jj * quarter, quarter), quarter)
        for part in range(parts):
            acc[part] += jnp.dot(held, wcat[part, depth, :], preferred_element_type=jnp.float32)

    def forward(blocks):
        for db in blocks:
            for k, at in enumerate(others):
                mm, yy = behind(*at)
                slot = x_buf.at[mm, yy * CORES + c, db]
                arrive(slot, a_s.at[db, k], a_r.at[db, k])
                start(slot, slot, b_s.at[db, k], b_r.at[db, k], partner)

    def experts(st, blocks):
        if st == 0:
            for copy in weights:
                copy.wait()
        acc[...] = jnp.zeros_like(acc)
        for dy in range(rows_tp):
            project(lax.rem(y + rows_tp - dy, rows_tp) * CORES + c, blocks)
        if st == 0:
            for d in range(1, ep_size):
                arrive(wr_buf.at[lax.rem(e + ep_size - d, ep_size)], wt_s.at[d], wt_r.at[d])
        for dy in range(rows_tp):
            for dm in range(members):
                mm, yy = behind(dm, dy)
                for db in blocks:
                    k = chunk_of[dm, dy]
                    slot = x_buf.at[mm, yy * CORES + (1 - c), db]
                    arrive(slot, b_s.at[db, k], b_r.at[db, k])
            project(lax.rem(y + rows_tp - dy, rows_tp) * CORES + (1 - c), blocks)
        hidden, scale = [], []
        for le in range(local):
            at, to = 2 * le * units, (2 * le + 1) * units
            gate = acc[at // width, :, at % width : at % width + units]
            up = acc[to // width, :, to % width : to % width + units]
            hidden.append((gate / (1.0 + jnp.exp(-gate)) * up).astype(jnp.bfloat16))
            columns = []
            for dm in range(members):
                for db in blocks:
                    source = block_at(db) * members + lax.rem(m + dm, members)
                    row = wr_buf[source, pl.ds(m * local + le, 1), :]
                    columns.append(jnp.sum(jnp.where(diagonal, row, 0.0), axis=1, keepdims=True))
            scale.append(jnp.concatenate(columns, axis=0))

        def lower(q):
            total = None
            for le in range(local):
                term = scale[le] * jnp.dot(
                    hidden[le], wdn[q, le], preferred_element_type=jnp.float32
                )
                total = term if total is None else total + term
            return total

        for dy in reversed(range(rows_tp)):
            q = lax.rem(y + dy, rows_tp) * CORES
            r1_send[st, dy] = lower(q + (1 - c))
            start(
                r1_send.at[st, dy], r1_recv.at[st, dy], c1_s.at[st, dy], c1_r.at[st, dy], partner
            )
        for dy in reversed(range(rows_tp)):
            q = lax.rem(y + dy, rows_tp) * CORES
            r1_own[st, dy] = lower(q + c)

    def summed(st, dm, dy):
        at = pl.ds(dm * rows, rows)
        return r1_own[st, dy, at, :] + r1_recv[st, dy, at, :]

    def reduce_send(st):
        for dy in reversed(range(rows_tp)):
            arrive(r1_recv.at[st, dy], c1_s.at[st, dy], c1_r.at[st, dy])
            for dm in reversed(range(members)):
                if not (dm or dy):
                    continue
                k = chunk_of[dm, dy]
                value = summed(st, dm, dy)
                top = jnp.maximum(jnp.max(jnp.abs(value), axis=1, keepdims=True), 1e-30)
                code = jnp.round(value * (LEVELS / top)).astype(jnp.int32).astype(jnp.int16)
                q_send[st, k] = code.reshape(per_stage, half, quarter)
                step = jnp.sum(
                    jnp.where(scale_eye, top * (1.0 / LEVELS), 0.0), axis=0, keepdims=True
                )
                u_send[st, k] = jnp.broadcast_to(step, u_send.shape[2:])
                start(
                    u_send.at[st, k], u_recv.at[st, k], cu_s.at[st, k], cu_r.at[st, k],
                    member(dm, dy),
                )
                for i in range(per_stage):
                    start(
                        q_send.at[st, k, i], q_recv.at[st, k, i],
                        c2_s.at[st, k, i], c2_r.at[st, k, i], member(dm, dy),
                    )

    def reduce_recv(st, blocks):
        total = summed(st, 0, 0)
        steps = []
        for k in range(own):
            arrive(u_recv.at[st, k], cu_s.at[st, k], cu_r.at[st, k])
            row = u_recv[st, k, 0:1, :]
            steps.append(jnp.sum(jnp.where(scale_eye, row, 0.0), axis=1, keepdims=True))
        for i, db in enumerate(blocks):
            at = slice(i * half, (i + 1) * half)
            block = total[at]
            for k in range(own):
                arrive(q_recv.at[st, k, i], c2_s.at[st, k, i], c2_r.at[st, k, i])
                code = q_recv[st, k, i].astype(jnp.int32).astype(jnp.float32)
                block = block + code * steps[k][at]
            f_send[db] = block.astype(jnp.bfloat16)
            if db:
                start(
                    f_send.at[db], f_recv.at[gme], c3_s.at[db], c3_r.at[db],
                    {"ep": block_at(db) * members + m, "tp": j},
                )
            else:
                f_recv[gme] = f_send[0]

    stages = [range(st * per_stage, (st + 1) * per_stage) for st in range(STAGES)]
    for st, blocks in enumerate(stages):
        forward(blocks)
        experts(st, blocks)
        if st:
            reduce_send(st)
            reduce_recv(st - 1, stages[st - 1])
        else:
            reduce_send(st)
    reduce_recv(STAGES - 1, stages[-1])
    for db in range(1, GROUPS):
        arrive(f_recv.at[lax.rem(gme + db, GROUPS)], c3_s.at[db], c3_r.at[db])
    out_ref[...] = jnp.dot(
        sel_buf[...], f_recv[...].reshape(lanes, quarter), preferred_element_type=jnp.float32
    ).astype(jnp.bfloat16)
    for copy in sent:
        copy.wait_send()


def per_device(tokens, norm_gain, norm_shift, expert_ids, gate_weights, w_gate, w_up, w_down):
    ep_size, tp_size = lax.axis_size("ep"), lax.axis_size("tp")
    tok_rows, features = tokens.shape
    local, _, units = w_gate.shape
    members, rows_tp = ep_size // GROUPS, tp_size // CORES
    half, quarter = tok_rows // 2, features // tp_size
    lanes = GROUPS * half
    group_size = local * members
    padded = -(-group_size // 8) * 8
    chunks = members * rows_tp
    parts, width = (1, 2 * local * units) if units % 128 == 0 else (2 * local, units)
    bf16, f32 = jnp.bfloat16, jnp.float32
    dma = pltpu.SemaphoreType.DMA
    vmem = pl.BlockSpec(memory_space=pltpu.VMEM)
    hbm = pl.BlockSpec(memory_space=pltpu.MemorySpace.HBM)
    per_stage = GROUPS // STAGES
    rows = per_stage * half
    all_rows = members * rows
    scale_lanes = -(-rows // 128) * 128
    return pl.pallas_call(
        functools.partial(kernel, ep_size, tp_size),
        out_shape=jax.ShapeDtypeStruct((tok_rows, quarter), bf16),
        in_specs=[hbm] * 8,
        out_specs=vmem,
        scratch_shapes=[
            pltpu.VMEM((tok_rows, features), bf16),
            pltpu.VMEM((1, features), f32),
            pltpu.VMEM((1, features), f32),
            pltpu.VMEM((expert_ids.shape[1], tok_rows), jnp.int32),
            pltpu.VMEM((expert_ids.shape[1], tok_rows), f32),
            pltpu.VMEM((members, tp_size, GROUPS, half, quarter), bf16),
            pltpu.VMEM((GROUPS, half, quarter), bf16),
            pltpu.VMEM((tok_rows, lanes), bf16),
            pltpu.VMEM((padded, lanes), f32),
            pltpu.VMEM((ep_size, padded, lanes), f32),
            pltpu.VMEM((parts, features, width), bf16),
            pltpu.VMEM((tp_size, local, units, quarter), bf16),
            pltpu.VMEM((parts, all_rows, width), f32),
            pltpu.VMEM((STAGES, rows_tp, all_rows, quarter), f32),
            pltpu.VMEM((STAGES, rows_tp, all_rows, quarter), f32),
            pltpu.VMEM((STAGES, rows_tp, all_rows, quarter), f32),
            pltpu.VMEM((STAGES, chunks - 1, per_stage, half, quarter), jnp.int16),
            pltpu.VMEM((STAGES, chunks - 1, per_stage, half, quarter), jnp.int16),
            pltpu.VMEM((STAGES, chunks - 1, 8, scale_lanes), f32),
            pltpu.VMEM((STAGES, chunks - 1, 8, scale_lanes), f32),
            pltpu.VMEM((GROUPS, half, quarter), bf16),
            pltpu.VMEM((GROUPS, half, quarter), bf16),
            dma((5,)),
            dma((local * (2 + tp_size),)),
            dma((GROUPS,)), dma((GROUPS,)),
            dma((ep_size,)), dma((ep_size,)),
            dma((GROUPS, chunks)), dma((GROUPS, chunks)),
            dma((GROUPS, chunks)), dma((GROUPS, chunks)),
            dma((STAGES, rows_tp)), dma((STAGES, rows_tp)),
            dma((STAGES, chunks, per_stage)), dma((STAGES, chunks, per_stage)),
            dma((STAGES, chunks)), dma((STAGES, chunks)),
            dma((GROUPS,)), dma((GROUPS,)),
        ],
        compiler_params=pltpu.CompilerParams(
            collective_id=0, has_side_effects=True, vmem_limit_bytes=60 * 1024 * 1024
        ),
    )(
        tokens, norm_gain.reshape(1, features), norm_shift.reshape(1, features),
        expert_ids.T, gate_weights.T, w_gate, w_up, w_down,
    )


def solution(mesh):
    return jax.shard_map(
        per_device,
        mesh=mesh,
        in_specs=(
            P("ep", None),
            P(),
            P(),
            P("ep", None),
            P("ep", None),
            P("ep", None, "tp"),
            P("ep", None, "tp"),
            P("ep", "tp", None),
        ),
        out_specs=P("ep", "tp"),
        check_vma=False,
    )
```

```python
import functools

import jax
import jax.numpy as jnp
from jax import lax
from jax.experimental import pallas as pl
from jax.experimental.pallas import tpu as pltpu
from jax.sharding import PartitionSpec as P

GROUPS = 4
CORES = 2
STAGES = 2
LEVELS = 32000.0
EPSILON = 1e-05
MESH = pl.DeviceIdType.MESH


def kernel(
    ep_size, tp_size,
    tok_hbm, gain_hbm, shift_hbm, ids_hbm, gw_hbm, wg_ref, wu_ref, wd_ref, out_ref,
    tok_ref, gain_ref, shift_ref, ids_ref, gw_ref,
    x_buf, xs_buf, sel_buf, wall_buf, wr_buf, wcat, wdn, acc,
    r1_send, r1_recv, r1_own, q_send, q_recv, u_send, u_recv, f_send, f_recv,
    in_sem, w_sem, s1_s, s1_r, wt_s, wt_r, a_s, a_r, b_s, b_r,
    c1_s, c1_r, c2_s, c2_r, cu_s, cu_r, c3_s, c3_r,
):
    tok_rows, features = tok_ref.shape
    local, _, units = wg_ref.shape
    top_k = ids_ref.shape[0]
    members = ep_size // GROUPS
    rows_tp = tp_size // CORES
    group_size = local * members
    half = tok_rows // 2
    quarter = features // tp_size
    lanes = GROUPS * half
    parts, _, width = wcat.shape
    per_stage = GROUPS // STAGES
    rows = per_stage * half
    scale_lanes = u_send.shape[-1]

    e = lax.axis_index("ep")
    j = lax.axis_index("tp")
    gme, m = e // members, e % members
    y, c = j // CORES, j % CORES
    partner = {"ep": e, "tp": y * CORES + (1 - c)}
    others = [(dm, dy) for dy in reversed(range(rows_tp)) for dm in reversed(range(members)) if dm or dy]
    chunk_of = {at: k for k, at in enumerate(others)}
    own = len(others)
    chunk_of[0, 0] = own

    def ahead(dm, dy):
        return lax.rem(m + dm, members), lax.rem(y + dy, rows_tp)

    def behind(dm, dy):
        return lax.rem(m + members - dm, members), lax.rem(y + rows_tp - dy, rows_tp)

    def member(dm, dy):
        mm, yy = ahead(dm, dy)
        return {"ep": gme * members + mm, "tp": yy * CORES + c}

    def block_at(db):
        return lax.rem(gme + GROUPS - db, GROUPS)

    def remote(src, dst, ssem, rsem, dev):
        return pltpu.make_async_remote_copy(
            src_ref=src, dst_ref=dst, send_sem=ssem, recv_sem=rsem,
            device_id=dev, device_id_type=MESH,
        )

    sent = []

    def start(*args):
        copy = remote(*args)
        copy.start()
        sent.append(copy)

    def arrive(slot, ssem, rsem):
        remote(slot, slot, ssem, rsem, partner).wait_recv()

    inputs = [
        pltpu.make_async_copy(s, d, in_sem.at[i])
        for i, (s, d) in enumerate([
            (ids_hbm, ids_ref), (gw_hbm, gw_ref), (tok_hbm, tok_ref),
            (gain_hbm, gain_ref), (shift_hbm, shift_ref),
        ])
    ]
    for copy in inputs:
        copy.start()

    barrier = pltpu.get_barrier_semaphore()
    greeted = 0
    for d in range(1, ep_size):
        pl.semaphore_signal(
            barrier, inc=1, device_id={"ep": lax.rem(e + d, ep_size), "tp": j}, device_id_type=MESH
        )
        greeted += 1
    for dm, dy in others:
        if dy:
            pl.semaphore_signal(barrier, inc=1, device_id=member(dm, dy), device_id_type=MESH)
            greeted += 1
    pl.semaphore_signal(barrier, inc=1, device_id=partner, device_id_type=MESH)
    greeted += 1

    weights = []
    for le in range(local):
        for source, at in ((wg_ref, 2 * le * units), (wu_ref, (2 * le + 1) * units)):
            weights.append(
                (source.at[le], wcat.at[at // width, :, pl.ds(at % width, units)])
            )
        for q in range(tp_size):
            weights.append((wd_ref.at[le, :, pl.ds(q * quarter, quarter)], wdn.at[q, le]))
    weights = [pltpu.make_async_copy(s, d, w_sem.at[i]) for i, (s, d) in enumerate(weights)]
    for copy in weights:
        copy.start()

    for copy in inputs[:2]:
        copy.wait()
    square = (tok_rows, tok_rows)
    token_at = lax.broadcasted_iota(jnp.int32, square, 0)
    other_at = lax.broadcasted_iota(jnp.int32, square, 1)
    ids = [
        jnp.sum(jnp.where(token_at == other_at, ids_ref[k : k + 1, :], 0), axis=1, keepdims=True)
        for k in range(top_k)
    ]
    gw = [
        jnp.sum(jnp.where(token_at == other_at, gw_ref[k : k + 1, :], 0.0), axis=1, keepdims=True)
        for k in range(top_k)
    ]
    group_of = ids[0] // group_size
    lane = lax.broadcasted_iota(jnp.int32, (tok_rows, lanes), 1)
    in_group = group_of == lane // half
    rank = jnp.dot(
        (other_at < token_at).astype(jnp.float32).astype(jnp.bfloat16),
        in_group.astype(jnp.float32).astype(jnp.bfloat16),
        preferred_element_type=jnp.float32,
    )
    picked = in_group & (rank == (lane % half).astype(jnp.float32))
    sel = picked.astype(jnp.float32)
    sel_bf = sel.astype(jnp.bfloat16)
    sel_buf[...] = sel_bf

    for copy in inputs[2:]:
        copy.wait()
    values = tok_ref[...].astype(jnp.float32)
    centre = jnp.mean(values, axis=-1, keepdims=True)
    spread = jnp.mean(jnp.square(values - centre), axis=-1, keepdims=True)
    share = pl.ds(pl.multiple_of(j * quarter, quarter), quarter)
    part = tok_ref[:, share].astype(jnp.float32)
    normed = (
        (part - centre) * lax.rsqrt(spread + EPSILON) * gain_ref[:, share] + shift_ref[:, share]
    ).astype(jnp.bfloat16)
    packed = lax.dot_general(
        sel_bf, normed, (((0,), (0,)), ((), ())), preferred_element_type=jnp.float32
    ).astype(jnp.bfloat16)
    xs_buf[...] = packed.reshape(GROUPS, half, quarter)

    pl.semaphore_wait(barrier, greeted)

    for dg in range(1, GROUPS):
        g = lax.rem(gme + dg, GROUPS)
        start(
            xs_buf.at[g], x_buf.at[m, j, dg], s1_s.at[dg], s1_r.at[dg],
            {"ep": g * members + m, "tp": j},
        )
    x_buf[m, j, 0] = xs_buf[gme]

    def spread_block(db):
        mine = x_buf.at[m, j, db]
        for k, (dm, dy) in enumerate(others):
            start(mine, mine, a_s.at[db, k], a_r.at[db, k], member(dm, dy))
        start(mine, mine, b_s.at[db, own], b_r.at[db, own], partner)

    spread_block(0)
    wall_buf[...] = jnp.zeros_like(wall_buf)
    for i in range(group_size):
        mine = 0.0
        for k in range(top_k):
            mine = mine + jnp.where(ids[k] - group_of * group_size == i, gw[k], 0.0)
        wall_buf[i : i + 1, :] = jnp.sum(sel * mine, axis=0, keepdims=True)
    for d in range(1, ep_size):
        start(
            wall_buf, wr_buf.at[e], wt_s.at[d], wt_r.at[d],
            {"ep": lax.rem(e + d, ep_size), "tp": j},
        )
    wr_buf[e] = wall_buf[...]
    for db in range(1, GROUPS):
        arrive(x_buf.at[m, j, db], s1_s.at[db], s1_r.at[db])
        spread_block(db)

    slot_row = lax.broadcasted_iota(jnp.int32, (half, lanes), 0) + gme * half
    diagonal = slot_row == lax.broadcasted_iota(jnp.int32, (half, lanes), 1)
    scale_eye = (
        lax.broadcasted_iota(jnp.int32, (rows, scale_lanes), 0)
        == lax.broadcasted_iota(jnp.int32, (rows, scale_lanes), 1)
    )

    def project(jj, blocks):
        held = [
            x_buf[lax.rem(m + dm, members), jj, db] for dm in range(members) for db in blocks
        ]
        held = jnp.concatenate(held, axis=0)
        depth = pl.ds(pl.multiple_of(jj * quarter, quarter), quarter)
        for part in range(parts):
            acc[part] += jnp.dot(held, wcat[part, depth, :], preferred_element_type=jnp.float32)

    def forward(blocks):
        for db in blocks:
            for k, at in enumerate(others):
                mm, yy = behind(*at)
                slot = x_buf.at[mm, yy * CORES + c, db]
                arrive(slot, a_s.at[db, k], a_r.at[db, k])
                start(slot, slot, b_s.at[db, k], b_r.at[db, k], partner)

    def experts(st, blocks):
        if st == 0:
            for copy in weights:
                copy.wait()
        acc[...] = jnp.zeros_like(acc)
        for dy in range(rows_tp):
            project(lax.rem(y + rows_tp - dy, rows_tp) * CORES + c, blocks)
        if st == 0:
            for d in range(1, ep_size):
                arrive(wr_buf.at[lax.rem(e + ep_size - d, ep_size)], wt_s.at[d], wt_r.at[d])
        for dy in range(rows_tp):
            for dm in range(members):
                mm, yy = behind(dm, dy)
                for db in blocks:
                    k = chunk_of[dm, dy]
                    slot = x_buf.at[mm, yy * CORES + (1 - c), db]
                    arrive(slot, b_s.at[db, k], b_r.at[db, k])
            project(lax.rem(y + rows_tp - dy, rows_tp) * CORES + (1 - c), blocks)
        hidden, scale = [], []
        for le in range(local):
            at, to = 2 * le * units, (2 * le + 1) * units
            gate = acc[at // width, :, at % width : at % width + units]
            up = acc[to // width, :, to % width : to % width + units]
            hidden.append((gate / (1.0 + jnp.exp(-gate)) * up).astype(jnp.bfloat16))
            columns = []
            for dm in range(members):
                for db in blocks:
                    source = block_at(db) * members + lax.rem(m + dm, members)
                    row = wr_buf[source, pl.ds(m * local + le, 1), :]
                    columns.append(jnp.sum(jnp.where(diagonal, row, 0.0), axis=1, keepdims=True))
            scale.append(jnp.concatenate(columns, axis=0))

        def lower(q):
            total = None
            for le in range(local):
                term = scale[le] * jnp.dot(
                    hidden[le], wdn[q, le], preferred_element_type=jnp.float32
                )
                total = term if total is None else total + term
            return total

        for dy in reversed(range(rows_tp)):
            q = lax.rem(y + dy, rows_tp) * CORES
            r1_send[st, dy] = lower(q + (1 - c))
            start(
                r1_send.at[st, dy], r1_recv.at[st, dy], c1_s.at[st, dy], c1_r.at[st, dy], partner
            )
        for dy in reversed(range(rows_tp)):
            q = lax.rem(y + dy, rows_tp) * CORES
            r1_own[st, dy] = lower(q + c)

    def summed(st, dm, dy):
        at = pl.ds(dm * rows, rows)
        return r1_own[st, dy, at, :] + r1_recv[st, dy, at, :]

    def reduce_send(st):
        for dy in reversed(range(rows_tp)):
            arrive(r1_recv.at[st, dy], c1_s.at[st, dy], c1_r.at[st, dy])
            for dm in reversed(range(members)):
                if not (dm or dy):
                    continue
                k = chunk_of[dm, dy]
                value = summed(st, dm, dy)
                top = jnp.maximum(jnp.max(jnp.abs(value), axis=1, keepdims=True), 1e-30)
                code = jnp.round(value * (LEVELS / top)).astype(jnp.int32).astype(jnp.int16)
                q_send[st, k] = code.reshape(per_stage, half, quarter)
                step = jnp.sum(
                    jnp.where(scale_eye, top * (1.0 / LEVELS), 0.0), axis=0, keepdims=True
                )
                u_send[st, k] = jnp.broadcast_to(step, u_send.shape[2:])
                start(
                    u_send.at[st, k], u_recv.at[st, k], cu_s.at[st, k], cu_r.at[st, k],
                    member(dm, dy),
                )
                for i in range(per_stage):
                    start(
                        q_send.at[st, k, i], q_recv.at[st, k, i],
                        c2_s.at[st, k, i], c2_r.at[st, k, i], member(dm, dy),
                    )

    def reduce_recv(st, blocks):
        total = summed(st, 0, 0)
        steps = []
        for k in range(own):
            arrive(u_recv.at[st, k], cu_s.at[st, k], cu_r.at[st, k])
            row = u_recv[st, k, 0:1, :]
            steps.append(jnp.sum(jnp.where(scale_eye, row, 0.0), axis=1, keepdims=True))
        for i, db in enumerate(blocks):
            at = slice(i * half, (i + 1) * half)
            block = total[at]
            for k in range(own):
                arrive(q_recv.at[st, k, i], c2_s.at[st, k, i], c2_r.at[st, k, i])
                code = q_recv[st, k, i].astype(jnp.int32).astype(jnp.float32)
                block = block + code * steps[k][at]
            f_send[db] = block.astype(jnp.bfloat16)
            if db:
                start(
                    f_send.at[db], f_recv.at[gme], c3_s.at[db], c3_r.at[db],
                    {"ep": block_at(db) * members + m, "tp": j},
                )
            else:
                f_recv[gme] = f_send[0]

    stages = [range(st * per_stage, (st + 1) * per_stage) for st in range(STAGES)]
    forward(stages[0])
    for st, blocks in enumerate(stages):
        experts(st, blocks)
        if st + 1 < STAGES:
            forward(stages[st + 1])
        reduce_send(st)
        if st:
            reduce_recv(st - 1, stages[st - 1])
    reduce_recv(STAGES - 1, stages[-1])
    for db in range(1, GROUPS):
        arrive(f_recv.at[lax.rem(gme + db, GROUPS)], c3_s.at[db], c3_r.at[db])
    out_ref[...] = jnp.dot(
        sel_buf[...], f_recv[...].reshape(lanes, quarter), preferred_element_type=jnp.float32
    ).astype(jnp.bfloat16)
    for copy in sent:
        copy.wait_send()


def per_device(tokens, norm_gain, norm_shift, expert_ids, gate_weights, w_gate, w_up, w_down):
    ep_size, tp_size = lax.axis_size("ep"), lax.axis_size("tp")
    tok_rows, features = tokens.shape
    local, _, units = w_gate.shape
    members, rows_tp = ep_size // GROUPS, tp_size // CORES
    half, quarter = tok_rows // 2, features // tp_size
    lanes = GROUPS * half
    group_size = local * members
    padded = -(-group_size // 8) * 8
    chunks = members * rows_tp
    parts, width = (1, 2 * local * units) if units % 128 == 0 else (2 * local, units)
    bf16, f32 = jnp.bfloat16, jnp.float32
    dma = pltpu.SemaphoreType.DMA
    vmem = pl.BlockSpec(memory_space=pltpu.VMEM)
    hbm = pl.BlockSpec(memory_space=pltpu.MemorySpace.HBM)
    per_stage = GROUPS // STAGES
    rows = per_stage * half
    all_rows = members * rows
    scale_lanes = -(-rows // 128) * 128
    return pl.pallas_call(
        functools.partial(kernel, ep_size, tp_size),
        out_shape=jax.ShapeDtypeStruct((tok_rows, quarter), bf16),
        in_specs=[hbm] * 8,
        out_specs=vmem,
        scratch_shapes=[
            pltpu.VMEM((tok_rows, features), bf16),
            pltpu.VMEM((1, features), f32),
            pltpu.VMEM((1, features), f32),
            pltpu.VMEM((expert_ids.shape[1], tok_rows), jnp.int32),
            pltpu.VMEM((expert_ids.shape[1], tok_rows), f32),
            pltpu.VMEM((members, tp_size, GROUPS, half, quarter), bf16),
            pltpu.VMEM((GROUPS, half, quarter), bf16),
            pltpu.VMEM((tok_rows, lanes), bf16),
            pltpu.VMEM((padded, lanes), f32),
            pltpu.VMEM((ep_size, padded, lanes), f32),
            pltpu.VMEM((parts, features, width), bf16),
            pltpu.VMEM((tp_size, local, units, quarter), bf16),
            pltpu.VMEM((parts, all_rows, width), f32),
            pltpu.VMEM((STAGES, rows_tp, all_rows, quarter), f32),
            pltpu.VMEM((STAGES, rows_tp, all_rows, quarter), f32),
            pltpu.VMEM((STAGES, rows_tp, all_rows, quarter), f32),
            pltpu.VMEM((STAGES, chunks - 1, per_stage, half, quarter), jnp.int16),
            pltpu.VMEM((STAGES, chunks - 1, per_stage, half, quarter), jnp.int16),
            pltpu.VMEM((STAGES, chunks - 1, 8, scale_lanes), f32),
            pltpu.VMEM((STAGES, chunks - 1, 8, scale_lanes), f32),
            pltpu.VMEM((GROUPS, half, quarter), bf16),
            pltpu.VMEM((GROUPS, half, quarter), bf16),
            dma((5,)),
            dma((local * (2 + tp_size),)),
            dma((GROUPS,)), dma((GROUPS,)),
            dma((ep_size,)), dma((ep_size,)),
            dma((GROUPS, chunks)), dma((GROUPS, chunks)),
            dma((GROUPS, chunks)), dma((GROUPS, chunks)),
            dma((STAGES, rows_tp)), dma((STAGES, rows_tp)),
            dma((STAGES, chunks, per_stage)), dma((STAGES, chunks, per_stage)),
            dma((STAGES, chunks)), dma((STAGES, chunks)),
            dma((GROUPS,)), dma((GROUPS,)),
        ],
        compiler_params=pltpu.CompilerParams(
            collective_id=0, has_side_effects=True, vmem_limit_bytes=60 * 1024 * 1024
        ),
    )(
        tokens, norm_gain.reshape(1, features), norm_shift.reshape(1, features),
        expert_ids.T, gate_weights.T, w_gate, w_up, w_down,
    )


def solution(mesh):
    return jax.shard_map(
        per_device,
        mesh=mesh,
        in_specs=(
            P("ep", None),
            P(),
            P(),
            P("ep", None),
            P("ep", None),
            P("ep", None, "tp"),
            P("ep", None, "tp"),
            P("ep", "tp", None),
        ),
        out_specs=P("ep", "tp"),
        check_vma=False,
    )
```
